256 devices in a mesh: sp: 32 (over z, y), dp: 8 (over x, core).
Axes of the slice: x: 4, y: 4, z: 8, core: 2. Of those that a mesh axis runs over, the one named last changes fastest.
Arguments:
- queries: bfloat16 [32, 16, 2048, 128], P('dp', None, 'sp'), may hold values from -6 to 6
- key_maps: bfloat16 [32, 16, 2048, 128], P('dp', None, 'sp'), may hold values from -6 to 6
- value_rows: bfloat16 [32, 16, 2048, 128], P('dp', None, 'sp'), may hold values from -6 to 6
- gate_logits: bfloat16 [2048, 32, 2048], P('sp', 'dp'), may hold values from -6 to 6
- mix_lambda: float32 [16], replicated, may hold values from 0.3 to 0.8
- head_gain: float32 [128], replicated, may hold values from 0.1 to 1.9
- out_weight: bfloat16 [2048, 2048], P('sp', 'dp'), may hold values from -0.125 to 0.125
Outputs:
- projected: bfloat16 [2048, 32, 2048], P('sp', 'dp')
The draws below stay inside these ranges and needn't reach their ends.
All inputs are finite; a program needn't handle non-finite values.
Results may differ from the reference program's by a relative error of at most 0.0075.
Values may be sent and summed in bfloat16 or wider, within the bound.
A program may use at most 64 MiB of HBM per device.

```python
from functools import partial
import jax
import jax.numpy as jnp
from jax import lax

HEADS = 16
HEAD_DIM = 64
V_DIM = 128
STRETCH = 64
BLOCK = 512
D = 2048
LENGTH = 2048
BATCH = 32


def draw_pair(key):
    shape = (BATCH, HEADS, LENGTH, 2 * HEAD_DIM)
    query_key = jax.random.fold_in(key, 11)
    keymap_key = jax.random.fold_in(key, 12)
    query_vals = jnp.clip(1.3 * jax.random.normal(query_key, shape, jnp.float32), -6.0, 6.0)
    keymap_vals = jnp.clip(1.3 * jax.random.normal(keymap_key, shape, jnp.float32), -6.0, 6.0)
    return (query_vals, keymap_vals)


def draw_queries(key, part):
    return draw_pair(key)[0].astype(jnp.bfloat16)


def draw_key_maps(key, part):
    return draw_pair(key)[1].astype(jnp.bfloat16)


def levels(stream_key, extent, shards, smallest, largest):
    factor_of, own = 1.0, jax.random.fold_in(stream_key, 6)
    for position, parts in shards:
        draws = jnp.exp(jax.random.uniform(jax.random.fold_in(own, position), (parts,), jnp.float32, smallest / len(shards), largest / len(shards)))
        factor_of = factor_of * jnp.repeat(draws, extent[position] // parts).reshape([-1 if axis == position else 1 for axis in range(len(extent))])
    return factor_of


def scatter_about(stream_key, shape, spread, reach, pieces=(), dtype=jnp.bfloat16):
    entries = spread * jax.random.normal(stream_key, shape, jnp.float32)
    if pieces:
        entries = entries * levels(stream_key, shape, pieces, -0.22, 0.18)
    return jnp.clip(entries, -reach, reach).astype(dtype)


def setup_inputs(seed: int = 0) -> dict:
    key_of = jax.random.split(jax.random.key(seed), 8)
    queries = draw_queries(jax.random.fold_in(key_of[7], 71), 0)
    key_maps = draw_key_maps(jax.random.fold_in(key_of[7], 71), 0)
    value_rows = scatter_about(key_of[2], (BATCH, HEADS, LENGTH, V_DIM), 1.0, 6.0, ((0, 8), (2, 32)))
    gate_logits = scatter_about(key_of[3], (LENGTH, BATCH, D), 1.0, 6.0, ((0, 32), (1, 8)))
    mix_lambda = jnp.clip(jax.random.uniform(key_of[4], (HEADS,), jnp.float32, 0.3, 0.8), 0.3, 0.8)
    head_gain = jnp.clip(1.0 + 0.18 * jax.random.normal(key_of[5], (V_DIM,), jnp.float32), 0.1, 1.9)
    out_weight = scatter_about(key_of[6], (D, D), D ** -0.5, 0.125, ((0, 32), (1, 8)))
    return dict(queries=queries, key_maps=key_maps, value_rows=value_rows, gate_logits=gate_logits, mix_lambda=mix_lambda, head_gain=head_gain, out_weight=out_weight)


def attend_item(operands, segment_ids, head_gain):
    query_item, key_item, value_item, weight_two = operands
    block_len = min(BLOCK, LENGTH)
    score_scale = HEAD_DIM ** (-0.5)
    outputs = []
    for block_index in range(LENGTH // block_len):
        offset = block_index * block_len
        limit = offset + block_len
        query_rows = query_item[offset:limit]
        key_block = key_item[:limit]
        value_block = value_item[:limit]
        visible = segment_ids[None, :limit] <= segment_ids[offset:limit, None]
        mapped = []
        for which in range(2):
            column_span = slice(which * HEAD_DIM, (which + 1) * HEAD_DIM)
            scores = jnp.dot(query_rows[:, column_span], key_block[:, column_span].T, preferred_element_type=jnp.float32) * score_scale
            scores = jnp.where(visible, scores, -1e+30)
            weights = jnp.exp(scores - lax.optimization_barrier(jnp.max(scores, axis=1, keepdims=True)))
            summed = lax.optimization_barrier(jnp.sum(weights, axis=1, keepdims=True))
            product = jnp.dot(weights.astype(jnp.bfloat16), value_block, preferred_element_type=jnp.float32)
            mapped.append(product / summed)
        combined = mapped[0] - weight_two * mapped[1]
        mean_sq = lax.optimization_barrier(jnp.mean(combined * combined, axis=1, keepdims=True))
        outputs.append((combined * lax.rsqrt(mean_sq + 1e-05) * head_gain).astype(jnp.bfloat16))
    return jnp.concatenate(outputs, axis=0)

def reference(queries, key_maps, value_rows, gate_logits, mix_lambda, head_gain, out_weight):
    item_count = BATCH * HEADS
    segment_ids = (jnp.arange(LENGTH) // STRETCH).astype(jnp.int32)
    lambda_items = jnp.tile(mix_lambda, BATCH)
    normed = lax.map(partial(attend_item, segment_ids=segment_ids, head_gain=head_gain), (queries.reshape(item_count, LENGTH, 2 * HEAD_DIM), key_maps.reshape(item_count, LENGTH, 2 * HEAD_DIM), value_rows.reshape(item_count, LENGTH, V_DIM), lambda_items))
    by_token = jnp.transpose(normed.reshape(BATCH, HEADS, LENGTH, V_DIM), (2, 0, 1, 3)).reshape(LENGTH, BATCH, D)
    gated = (jax.nn.sigmoid(gate_logits.astype(jnp.float32)) * by_token.astype(jnp.float32)).astype(jnp.bfloat16)
    output = jnp.dot(gated.reshape(LENGTH * BATCH, D), out_weight, preferred_element_type=jnp.float32)
    return output.astype(jnp.bfloat16).reshape(LENGTH, BATCH, D)
```

```python
import functools
import math

import jax
import jax.numpy as jnp
from jax import lax
from jax.experimental import pallas as pl
from jax.experimental.pallas import tpu as pltpu
from jax.sharding import PartitionSpec as P

MESH = pl.DeviceIdType.MESH
HEAD_DIM = 64
NZ, NY, NX = 8, 4, 4
NSP, NDP = NZ * NY, 2 * NX
EXP_SCALE = HEAD_DIM ** (-0.5) * math.log2(math.e)
F32, BF16 = jnp.float32, jnp.bfloat16


def slab_offset(step):
    half = (step + 1) // 2
    return jnp.where(step % 2 == 1, half, lax.rem(NZ - half, NZ))


def slab_attention(s, item, recv, vt, scores, ostage, lam, gain):
    lane = lax.broadcasted_iota(jnp.int32, (128, 128), 1)
    half_lane = lax.rem(lax.broadcasted_iota(jnp.int32, (64, 256), 1), 128)
    for h in range(2):
        first = NY * s + 2 * h
        q = recv[item, pl.ds(first, 2), 2].reshape(128, 128)
        zero = jnp.zeros_like(q)
        qm = jnp.concatenate(
            [jnp.where(lane < HEAD_DIM, q, zero), jnp.where(lane >= HEAD_DIM, q, zero)], axis=0
        )
        chunks = first + 2
        blocks = []
        at = 0
        while at < chunks:
            size = min(4, chunks - at)
            blocks.append((at, size))
            at += size
        highest = jnp.full((8, 256), -1e30, F32)
        for at, size in blocks:
            rows = 64 * size
            keys = recv[item, pl.ds(at, size), 0].reshape(rows, 128)
            st = lax.dot_general(
                keys, qm, (((1,), (1,)), ((), ())), preferred_element_type=F32
            )
            if at + size == chunks:
                tail = jnp.where(half_lane < 64, -1e30, st[rows - 64 :])
                st = jnp.concatenate([st[: rows - 64], tail], axis=0)
            scores[h, pl.ds(64 * at, rows)] = st
            highest = jnp.maximum(highest, jnp.max(st.reshape(rows // 8, 8, 256), axis=0))
        highest = jnp.max(highest, axis=0, keepdims=True)
        summed = jnp.zeros((8, 256), F32)
        mapped = jnp.zeros((128, 256), F32)
        for at, size in blocks:
            rows = 64 * size
            weights = jnp.exp2((scores[h, pl.ds(64 * at, rows)] - highest) * EXP_SCALE)
            summed = summed + jnp.sum(weights.reshape(rows // 8, 8, 256), axis=0)
            mapped = mapped + jnp.dot(
                vt[:, pl.ds(64 * at, rows)], weights.astype(BF16), preferred_element_type=F32
            )
        mapped = mapped * (1.0 / jnp.sum(summed, axis=0, keepdims=True))
        combined = mapped[:, :128] - lam * mapped[:, 128:]
        mean_sq = jnp.sum(combined * combined, axis=0, keepdims=True) * (1.0 / 128)
        normed = (combined * lax.rsqrt(mean_sq + 1e-5)).T * gain
        ostage[item, pl.ds(first, 2)] = normed.astype(BF16).reshape(2, 64, 128)


def kernel(
    q_hbm, k_hbm, v_hbm, gate_hbm, lam_ref, gain_ref, w_hbm, out_ref,
    src, recv, vt, scores, ostage, orecv, wall, gate, sig, gated,
    load_sem, gate_sem, wload_sem, kv_send, kv_recv, q_recv, o_send, o_recv,
    wz_send, wz_recv, wy_send, wy_recv, wx_send, wx_recv, wp_send, wp_recv,
):
    me = lax.axis_index("sp")
    dp = lax.axis_index("dp")
    z, y = me // NY, lax.rem(me, NY)
    x, core = dp // 2, lax.rem(dp, 2)

    def plane_peer(dz, dy):
        return lax.rem(z + dz, NZ) * NY + lax.rem(y + dy, NY)

    def x_peer(dx):
        return lax.rem(x + dx, NX) * 2 + core

    partner = x * 2 + 1 - core
    barrier = pltpu.get_barrier_semaphore()

    @pl.loop(1, NSP)
    def _(d):
        pl.semaphore_signal(
            barrier, inc=1, device_id=(lax.rem(me + d, NSP), dp), device_id_type=MESH
        )

    @pl.loop(1, NX)
    def _(d):
        pl.semaphore_signal(barrier, inc=1, device_id=(me, x_peer(d)), device_id_type=MESH)

    pl.semaphore_signal(barrier, inc=1, device_id=(me, partner), device_id_type=MESH)

    def local(a, b, sem):
        copy = pltpu.make_async_copy(a, b, sem)
        copy.start()
        return copy

    tensors = (k_hbm, v_hbm, q_hbm)
    w_load = local(w_hbm, wall.at[dp, z, y], wload_sem)
    loads = []
    for i in range(2):
        loads.append(
            [
                local(t.at[pl.ds(NSP * i, NSP)], src.at[pl.ds(NSP * i, NSP), n], load_sem.at[i, n])
                for n, t in enumerate(tensors)
            ]
        )
        for n, t in enumerate(tensors):
            local(
                t.at[NSP * i + me],
                recv.at[i, me, n],
                kv_recv.at[i] if n < 2 else q_recv.at[i, z],
            )
    gate_load = local(gate_hbm, gate, gate_sem)

    w_load.wait()
    pl.semaphore_wait(barrier, NSP - 1 + NX - 1 + 1)

    def remote(a, b, send, rcv, sp, d):
        copy = pltpu.make_async_remote_copy(
            src_ref=a, dst_ref=b, send_sem=send, recv_sem=rcv, device_id=(sp, d), device_id_type=MESH
        )
        copy.start()

    def drain(ref, sem):
        pltpu.make_async_copy(ref, ref, sem).wait()

    @pl.loop(1, NZ)
    def _(d):
        block = wall.at[dp, z, y]
        remote(block, block, wz_send, wz_recv, plane_peer(d, 0), dp)

    def send_inputs(i, start, count, rcv):
        @pl.loop(0, NSP)
        def _(n):
            dz, dy = slab_offset(n // NY), lax.rem(n, NY)

            @pl.when(n > 0)
            def _():
                to = plane_peer(dz, dy)
                remote(
                    src.at[NSP * i + to, pl.ds(start, count)],
                    recv.at[i, me, pl.ds(start, count)],
                    kv_send,
                    rcv,
                    to,
                    dp,
                )

    for i in range(2):
        for copy in loads[i][:2]:
            copy.wait()
        send_inputs(i, 0, 2, kv_recv.at[i])
        loads[i][2].wait()
        send_inputs(i, 2, 1, q_recv.at[i, z])
        if i == 0:
            drain(wall.at[dp, pl.ds(0, NZ - 1), y], wz_recv)
            mine = wall.at[dp, :, y]

            @pl.loop(1, NY)
            def _(d):
                remote(mine, mine, wy_send, wy_recv, plane_peer(0, d), dp)

            @pl.loop(1, NX)
            def _(d):
                remote(mine, mine, wx_send, wx_recv, me, x_peer(d))

    gate_load.wait()
    for b in range(4):
        sig[b] = jax.nn.sigmoid(gate[b].astype(F32))

    lam = lam_ref[lax.rem(me, 16)]
    gain = gain_ref[...]

    @pl.loop(0, 2)
    def _(item):
        drain(recv.at[0, :, pl.ds(0, 2)], kv_recv.at[item])

        @pl.loop(0, NZ)
        def _(b):
            cols = pl.ds(pl.multiple_of(256 * b, 256), 256)
            vt[:, cols] = recv[item, pl.ds(NY * b, NY), 1].reshape(256, 128).T

        @pl.loop(0, NZ)
        def _(step):
            slab = lax.rem(z + NZ - slab_offset(step), NZ)
            drain(recv.at[0, pl.ds(0, NY), 2], q_recv.at[item, slab])
            for s in range(NZ):

                @pl.when(slab == s)
                def _():
                    slab_attention(s, item, recv, vt, scores, ostage, lam, gain)

            @pl.loop(0, NY)
            def _(n):
                to = slab * NY + n

                @pl.when(to == me)
                def _():
                    orecv[NSP * item + me] = ostage[item, me]

                @pl.when(to != me)
                def _():
                    remote(
                        ostage.at[item, to], orecv.at[NSP * item + me], o_send, o_recv.at[item], to, dp
                    )

        @pl.when(item == 0)
        def _():
            drain(wall.at[dp, :, pl.ds(0, NY - 1)], wy_recv)

            @pl.loop(1, NY)
            def _(dy):
                rows = wall.at[dp, :, lax.rem(y + dy, NY)]

                @pl.loop(1, NX)
                def _(d):
                    remote(rows, rows, wx_send, wx_recv, me, x_peer(d))

            remote(wall.at[dp], wall.at[dp], wp_send, wp_recv, me, partner)

    drain(wall.at[pl.ds(0, NX - 1)], wx_recv)

    @pl.loop(1, NX)
    def _(d):
        rows = wall.at[x_peer(d)]
        remote(rows, rows, wp_send, wp_recv, me, partner)

    for i in range(2):
        drain(orecv.at[pl.ds(0, NSP - 1)], o_recv.at[i])

        @pl.loop(0, 16)
        def _(h):
            cols = pl.ds(pl.multiple_of(128 * h, 128), 128)
            for b in (2 * i, 2 * i + 1):
                gated[pl.ds(64 * b, 64), cols] = (
                    sig[b, :, cols] * orecv[16 * b + h].astype(F32)
                ).astype(BF16)

    drain(wall.at[pl.ds(0, NX)], wp_recv)

    @pl.loop(0, NDP)
    def _(c):
        cols = pl.ds(pl.multiple_of(256 * c, 256), 256)
        out_ref[:, cols] = jnp.dot(
            gated[...], wall[c].reshape(2048, 256), preferred_element_type=F32
        ).astype(BF16)

    drain(src.at[pl.ds(0, 2 * (NSP - 1))], kv_send)
    drain(ostage.at[0, pl.ds(0, NSP - 1)], o_send)
    drain(ostage.at[0, pl.ds(0, NSP - 1)], o_send)
    drain(wall.at[dp, pl.ds(0, NZ - 1), y], wz_send)
    drain(wall.at[dp, :, pl.ds(0, NY - 1)], wy_send)
    drain(wall.at[pl.ds(0, NX - 1)], wx_send)
    drain(wall.at[pl.ds(0, NX)], wp_send)


def on_device(queries, key_maps, value_rows, gate_logits, mix_lambda, head_gain, out_weight):
    items = 64
    any_spec = pl.BlockSpec(memory_space=pl.ANY)
    dma = pltpu.SemaphoreType.DMA
    gate_by_seq = jnp.transpose(gate_logits, (1, 0, 2))
    out = pl.pallas_call(
        kernel,
        out_shape=jax.ShapeDtypeStruct((256, 2048), BF16),
        in_specs=[any_spec, any_spec, any_spec, any_spec, pl.BlockSpec(memory_space=pltpu.SMEM),
                  pl.BlockSpec(memory_space=pltpu.VMEM), any_spec],
        out_specs=pl.BlockSpec(memory_space=pltpu.VMEM),
        scratch_shapes=[
            pltpu.VMEM((items, 3, 64, 128), BF16),
            pltpu.VMEM((2, NSP, 3, 64, 128), BF16),
            pltpu.VMEM((128, 2048), BF16),
            pltpu.VMEM((2, 2048, 256), F32),
            pltpu.VMEM((2, NSP, 64, 128), BF16),
            pltpu.VMEM((items, 64, 128), BF16),
            pltpu.VMEM((NDP, NZ, NY, 64, 256), BF16),
            pltpu.VMEM((4, 64, 2048), BF16),
            pltpu.VMEM((4, 64, 2048), F32),
            pltpu.VMEM((256, 2048), BF16),
            dma((2, 3)), dma, dma, dma, dma((2,)), dma((2, NZ)), dma, dma((2,)),
            dma, dma, dma, dma, dma, dma, dma, dma,
        ],
        compiler_params=pltpu.CompilerParams(
            collective_id=0, has_side_effects=True, vmem_limit_bytes=60 << 20
        ),
        name="fused_layer",
    )(
        queries.reshape(items, 64, 128),
        key_maps.reshape(items, 64, 128),
        value_rows.reshape(items, 64, 128),
        gate_by_seq,
        mix_lambda,
        head_gain.reshape(1, 128),
        out_weight,
    )
    return jnp.transpose(out.reshape(4, 64, 2048), (1, 0, 2))


def solution(mesh):
    return jax.shard_map(
        on_device,
        mesh=mesh,
        in_specs=(
            P("dp", None, "sp", None),
            P("dp", None, "sp", None),
            P("dp", None, "sp", None),
            P("sp", "dp", None),
            P(),
            P(),
            P("sp", "dp"),
        ),
        out_specs=P("sp", "dp", None),
        check_vma=False,
    )
```

```python
import math

import jax
import jax.numpy as jnp
from jax import lax
from jax.experimental import pallas as pl
from jax.experimental.pallas import tpu as pltpu
from jax.sharding import PartitionSpec as P

MESH = pl.DeviceIdType.MESH
HEAD_DIM = 64
NZ, NY, NX = 8, 4, 4
NSP, NDP = NZ * NY, 2 * NX
AHEAD_1, AHEAD_2 = 8, 14
EXP_SCALE = HEAD_DIM ** (-0.5) * math.log2(math.e)
F32, BF16 = jnp.float32, jnp.bfloat16


def slab_offset(step):
    return step // 2 + 4 * (step % 2)


def transpose_values(kvq, vt, block):
    cols = pl.ds(pl.multiple_of(256 * block, 256), 256)
    vt[:, cols] = kvq[pl.ds(NY * block, NY), 1].reshape(256, 128).T


def slab_attention(s, kvq, vt, scores, out, lam, gain):
    lane = lax.broadcasted_iota(jnp.int32, (128, 128), 1)
    half_lane = lax.rem(lax.broadcasted_iota(jnp.int32, (64, 256), 1), 128)
    for h in range(2):
        first = NY * s + 2 * h
        q = kvq[pl.ds(first, 2), 2].reshape(128, 128)
        zero = jnp.zeros_like(q)
        qm = jnp.concatenate(
            [jnp.where(lane < HEAD_DIM, q, zero), jnp.where(lane >= HEAD_DIM, q, zero)], axis=0
        )
        chunks = first + 2
        blocks = []
        at = 0
        while at < chunks:
            size = min(4, chunks - at)
            blocks.append((at, size))
            at += size
        highest = jnp.full((8, 256), -1e30, F32)
        for at, size in blocks:
            rows = 64 * size
            keys = kvq[pl.ds(at, size), 0].reshape(rows, 128)
            st = lax.dot_general(
                keys, qm, (((1,), (1,)), ((), ())), preferred_element_type=F32
            )
            if at + size == chunks:
                tail = jnp.where(half_lane < 64, -1e30, st[rows - 64 :])
                st = jnp.concatenate([st[: rows - 64], tail], axis=0)
            scores[h, pl.ds(64 * at, rows)] = st
            highest = jnp.maximum(highest, jnp.max(st.reshape(rows // 8, 8, 256), axis=0))
        highest = jnp.max(highest, axis=0, keepdims=True)
        summed = jnp.zeros((8, 256), F32)
        mapped = jnp.zeros((128, 256), F32)
        for at, size in blocks:
            rows = 64 * size
            weights = jnp.exp2((scores[h, pl.ds(64 * at, rows)] - highest) * EXP_SCALE)
            summed = summed + jnp.sum(weights.reshape(rows // 8, 8, 256), axis=0)
            mapped = mapped + jnp.dot(
                vt[:, pl.ds(64 * at, rows)], weights.astype(BF16), preferred_element_type=F32
            )
        mapped = mapped * (1.0 / jnp.sum(summed, axis=0, keepdims=True))
        combined = mapped[:, :128] - lam * mapped[:, 128:]
        mean_sq = jnp.sum(combined * combined, axis=0, keepdims=True) * (1.0 / 128)
        normed = (combined * lax.rsqrt(mean_sq + 1e-5)).T * gain
        out[pl.ds(first, 2)] = normed.astype(BF16).reshape(2, 64, 128)


def kernel(
    q_hbm, k_hbm, v_hbm, gate_hbm, lam_ref, gain_ref, w_hbm, out_ref,
    src, recv, vt, scores, ostage, orecv, wall, gate, mixed, sig, gated, acc,
    load_sem, gate_sem, wload_sem, kv_send, kv_recv, q_send, q_recv, o_send, o_recv,
    wz_send, wz_recv, wy_send, wy_recv, wx_send, wx_recv, wp_send, wp_recv,
):
    me = lax.axis_index("sp")
    dp = lax.axis_index("dp")
    z, y = me // NY, lax.rem(me, NY)
    x, core = dp // 2, lax.rem(dp, 2)

    def plane_peer(dz, dy):
        return lax.rem(z + dz, NZ) * NY + lax.rem(y + dy, NY)

    def x_peer(dx):
        return lax.rem(x + dx, NX) * 2 + core

    partner = x * 2 + 1 - core
    barrier = pltpu.get_barrier_semaphore()

    @pl.loop(1, NSP)
    def _(d):
        pl.semaphore_signal(
            barrier, inc=1, device_id=(lax.rem(me + d, NSP), dp), device_id_type=MESH
        )

    @pl.loop(1, NX)
    def _(d):
        pl.semaphore_signal(barrier, inc=1, device_id=(me, x_peer(d)), device_id_type=MESH)

    pl.semaphore_signal(barrier, inc=1, device_id=(me, partner), device_id_type=MESH)

    def local(a, b, sem):
        copy = pltpu.make_async_copy(a, b, sem)
        copy.start()
        return copy

    def remote(a, b, send, rcv, sp, d):
        copy = pltpu.make_async_remote_copy(
            src_ref=a, dst_ref=b, send_sem=send, recv_sem=rcv, device_id=(sp, d), device_id_type=MESH
        )
        copy.start()

    def drain(ref, sem):
        pltpu.make_async_copy(ref, ref, sem).wait()

    tensors = (k_hbm, v_hbm, q_hbm)
    w_load = local(w_hbm, wall.at[dp, z, y], wload_sem)
    loads = []
    for i in range(2):
        loads.append(
            [local(t.at[i], src.at[i, :, :, n], load_sem.at[i, n]) for n, t in enumerate(tensors)]
        )
        for n, t in enumerate(tensors):
            local(
                t.at[i, z, y],
                recv.at[i, me, n],
                kv_recv.at[i] if n < 2 else q_recv.at[i, z],
            )
    gate_load = local(gate_hbm, gate, gate_sem)

    w_load.wait()
    for i in range(2):
        for copy in loads[i]:
            copy.wait()
    pl.semaphore_wait(barrier, NSP - 1 + NX - 1 + 1)

    def send_weights_z(row, dz, rcv):
        block = wall.at[dp, row, y]
        remote(block, block, wz_send, rcv, plane_peer(dz, 0), dp)

    def send_weights_x(col):
        rows = wall.at[dp, :, col]

        @pl.loop(1, NX)
        def _(d):
            remote(rows, rows, wx_send, wx_recv, me, x_peer(d))

    def send_kv(i, start, stop):
        @pl.loop(start, stop)
        def _(n):
            to = plane_peer(slab_offset(n // NY), lax.rem(n, NY))
            remote(
                src.at[i, to // NY, lax.rem(to, NY), pl.ds(0, 2)],
                recv.at[i, me, pl.ds(0, 2)],
                kv_send,
                kv_recv.at[i],
                to,
                dp,
            )

    def send_q(i):
        @pl.loop(1, NSP)
        def _(n):
            to = plane_peer(slab_offset(n // NY), lax.rem(n, NY))
            remote(
                src.at[i, to // NY, lax.rem(to, NY), 2],
                recv.at[i, me, 2],
                q_send,
                q_recv.at[i, z],
                to,
                dp,
            )

    for dz in (1, NZ - 1, 2, NZ - 2):
        send_weights_z(z, dz, wz_recv.at[0])
    send_kv(0, 1, AHEAD_1)
    drain(wall.at[dp, pl.ds(0, 4), y], wz_recv.at[0])
    before, after = lax.rem(z + NZ - 2, NZ), lax.rem(z + 2, NZ)
    send_weights_z(before, 1, wz_recv.at[1])
    send_weights_z(before, 2, wz_recv.at[1])
    send_weights_z(after, NZ - 1, wz_recv.at[1])
    send_kv(0, AHEAD_1, AHEAD_2)
    drain(wall.at[dp, pl.ds(0, 3), y], wz_recv.at[1])

    @pl.loop(1, NY)
    def _(d):
        mine = wall.at[dp, :, y]
        remote(mine, mine, wy_send, wy_recv, plane_peer(0, d), dp)

    send_weights_x(y)
    send_kv(0, AHEAD_2, NSP)
    send_q(0)

    gate_load.wait()

    @pl.loop(0, 16)
    def _(n):
        rows = pl.ds(pl.multiple_of(4 * n, 4), 4)
        mixed[rows] = jax.nn.sigmoid(gate[rows].astype(F32))

    for b in range(4):
        sig[b] = mixed[:, b]

    drain(wall.at[dp, :, pl.ds(0, NY - 1)], wy_recv)

    @pl.loop(1, NY)
    def _(d):
        send_weights_x(lax.rem(y + d, NY))

    remote(wall.at[dp], wall.at[dp], wp_send, wp_recv, me, partner)
    send_kv(1, 1, NSP)
    send_q(1)

    gain = gain_ref[...]
    lam = lam_ref[lax.rem(me, 16)]

    @pl.loop(0, 2)
    def _(item):
        drain(recv.at[0, :, pl.ds(0, 2)], kv_recv.at[item])
        kvq = recv.at[item]

        @pl.loop(0, NZ)
        def _(b):
            transpose_values(kvq, vt, b)

        @pl.loop(0, NZ)
        def _(step):
            slab = lax.rem(z + NZ - slab_offset(step), NZ)
            drain(recv.at[0, pl.ds(0, NY), 2], q_recv.at[item, slab])
            for s in range(NZ):

                @pl.when(slab == s)
                def _():
                    slab_attention(s, kvq, vt, scores, ostage.at[item], lam, gain)

            @pl.loop(0, NY)
            def _(n):
                to = slab * NY + n

                @pl.when(to == me)
                def _():
                    orecv[item, z, y] = ostage[item, me]

                @pl.when(to != me)
                def _():
                    remote(
                        ostage.at[item, to],
                        orecv.at[item, z, y],
                        o_send,
                        o_recv.at[item, z],
                        to,
                        dp,
                    )

        @pl.when(item == 0)
        def _():
            drain(wall.at[pl.ds(0, NX - 1)], wx_recv)

            @pl.loop(1, NX)
            def _(d):
                rows = wall.at[x_peer(d)]
                remote(rows, rows, wp_send, wp_recv, me, partner)

    drain(wall.at[pl.ds(0, NX)], wp_recv)
    acc[...] = jnp.zeros_like(acc)

    @pl.loop(0, NZ)
    def _(step):
        i = step // 4
        j = lax.rem(z + step, 4)
        for b in range(2):
            rank = j + 4 * b

            @pl.when(rank == z)
            def _():
                drain(orecv.at[0, 0, pl.ds(0, NY - 1)], o_recv.at[i, rank])

            @pl.when(rank != z)
            def _():
                drain(orecv.at[0, 0], o_recv.at[i, rank])

            for h in range(4):
                cols = pl.ds(pl.multiple_of(512 * j + 128 * h, 128), 128)
                gated[pl.ds(64 * b, 64), pl.ds(128 * h, 128)] = (
                    sig[2 * i + b, :, cols] * orecv[i, rank, h].astype(F32)
                ).astype(BF16)
        for c in range(NDP):
            acc[i, :, pl.ds(256 * c, 256)] += jnp.dot(
                gated[...], wall[c, pl.ds(2 * j, 2)].reshape(512, 256), preferred_element_type=F32
            )

    out_ref[...] = acc[...].astype(BF16)

    drain(recv.at[:, pl.ds(0, NSP - 1), pl.ds(0, 2)], kv_send)
    drain(recv.at[:, pl.ds(0, NSP - 1), 2], q_send)
    drain(ostage.at[:, pl.ds(0, NSP - 1)], o_send)
    drain(wall.at[dp, pl.ds(0, NZ - 1), y], wz_send)
    drain(wall.at[dp, :, pl.ds(0, NY - 1)], wy_send)
    drain(wall.at[pl.ds(0, NX - 1)], wx_send)
    drain(wall.at[pl.ds(0, NX)], wp_send)


def on_device(queries, key_maps, value_rows, gate_logits, mix_lambda, head_gain, out_weight):
    any_spec = pl.BlockSpec(memory_space=pl.ANY)
    dma = pltpu.SemaphoreType.DMA
    out = pl.pallas_call(
        kernel,
        out_shape=jax.ShapeDtypeStruct((2, 128, 2048), BF16),
        in_specs=[any_spec, any_spec, any_spec, any_spec, pl.BlockSpec(memory_space=pltpu.SMEM),
                  pl.BlockSpec(memory_space=pltpu.VMEM), any_spec],
        out_specs=pl.BlockSpec(memory_space=pltpu.VMEM),
        scratch_shapes=[
            pltpu.VMEM((2, NZ, NY, 3, 64, 128), BF16),
            pltpu.VMEM((2, NSP, 3, 64, 128), BF16),
            pltpu.VMEM((128, 2048), BF16),
            pltpu.VMEM((2, 2048, 256), F32),
            pltpu.VMEM((2, NSP, 64, 128), BF16),
            pltpu.VMEM((2, NZ, NY, 64, 128), BF16),
            pltpu.VMEM((NDP, NZ, NY, 64, 256), BF16),
            pltpu.VMEM((64, 4, 2048), BF16),
            pltpu.VMEM((64, 4, 2048), F32),
            pltpu.VMEM((4, 64, 2048), F32),
            pltpu.VMEM((128, 512), BF16),
            pltpu.VMEM((2, 128, 2048), F32),
            dma((2, 3)), dma, dma, dma, dma((2,)), dma, dma((2, NZ)), dma, dma((2, NZ)),
            dma, dma((2,)), dma, dma, dma, dma, dma, dma,
        ],
        compiler_params=pltpu.CompilerParams(
            collective_id=0, has_side_effects=True, vmem_limit_bytes=60 << 20
        ),
        name="fused_layer",
    )(
        queries.reshape(2, NZ, NY, 64, 128),
        key_maps.reshape(2, NZ, NY, 64, 128),
        value_rows.reshape(2, NZ, NY, 64, 128),
        gate_logits,
        mix_lambda,
        head_gain.reshape(1, 128),
        out_weight,
    )
    return jnp.transpose(out.reshape(4, 64, 2048), (1, 0, 2))


def solution(mesh):
    return jax.shard_map(
        on_device,
        mesh=mesh,
        in_specs=(
            P("dp", None, "sp", None),
            P("dp", None, "sp", None),
            P("dp", None, "sp", None),
            P("sp", "dp", None),
            P(),
            P(),
            P("sp", "dp"),
        ),
        out_specs=P("sp", "dp", None),
        check_vma=False,
    )
```

```python
import math

import jax
import jax.numpy as jnp
from jax import lax
from jax.experimental import pallas as pl
from jax.experimental.pallas import tpu as pltpu
from jax.sharding import PartitionSpec as P

MESH = pl.DeviceIdType.MESH
HEAD_DIM = 64
NZ, NY, NX = 8, 4, 4
NSP, NDP = NZ * NY, 2 * NX
AHEAD_1, AHEAD_2 = 8, 14
LOCAL = 1
EXP_SCALE = HEAD_DIM ** (-0.5) * math.log2(math.e)
F32, BF16 = jnp.float32, jnp.bfloat16


def slab_offset(step):
    return step // 2 + 4 * (step % 2)


def transpose_values(kvq, vt, block):
    cols = pl.ds(pl.multiple_of(256 * block, 256), 256)
    vt[:, cols] = kvq[pl.ds(NY * block, NY), 1].reshape(256, 128).T


def slab_attention(s, kvq, vt, scores, out, lam, gain):
    lane = lax.broadcasted_iota(jnp.int32, (128, 128), 1)
    half_lane = lax.rem(lax.broadcasted_iota(jnp.int32, (64, 256), 1), 128)
    for h in range(2):
        first = NY * s + 2 * h
        q = kvq[pl.ds(first, 2), 2].reshape(128, 128)
        zero = jnp.zeros_like(q)
        qm = jnp.concatenate(
            [jnp.where(lane < HEAD_DIM, q, zero), jnp.where(lane >= HEAD_DIM, q, zero)], axis=0
        )
        chunks = first + 2
        blocks = []
        at = 0
        while at < chunks:
            size = min(4, chunks - at)
            blocks.append((at, size))
            at += size
        highest = jnp.full((8, 256), -1e30, F32)
        for at, size in blocks:
            rows = 64 * size
            keys = kvq[pl.ds(at, size), 0].reshape(rows, 128)
            st = lax.dot_general(
                keys, qm, (((1,), (1,)), ((), ())), preferred_element_type=F32
            )
            if at + size == chunks:
                tail = jnp.where(half_lane < 64, -1e30, st[rows - 64 :])
                st = jnp.concatenate([st[: rows - 64], tail], axis=0)
            scores[h, pl.ds(64 * at, rows)] = st
            highest = jnp.maximum(highest, jnp.max(st.reshape(rows // 8, 8, 256), axis=0))
        highest = jnp.max(highest, axis=0, keepdims=True)
        summed = jnp.zeros((8, 256), F32)
        mapped = jnp.zeros((128, 256), F32)
        for at, size in blocks:
            rows = 64 * size
            weights = jnp.exp2((scores[h, pl.ds(64 * at, rows)] - highest) * EXP_SCALE)
            summed = summed + jnp.sum(weights.reshape(rows // 8, 8, 256), axis=0)
            mapped = mapped + jnp.dot(
                vt[:, pl.ds(64 * at, rows)], weights.astype(BF16), preferred_element_type=F32
            )
        mapped = mapped * (1.0 / jnp.sum(summed, axis=0, keepdims=True))
        combined = mapped[:, :128] - lam * mapped[:, 128:]
        mean_sq = jnp.sum(combined * combined, axis=0, keepdims=True) * (1.0 / 128)
        normed = (combined * lax.rsqrt(mean_sq + 1e-5)).T * gain
        out[pl.ds(first, 2)] = normed.astype(BF16).reshape(2, 64, 128)


def kernel(
    q_hbm, k_hbm, v_hbm, gate_hbm, lam_ref, gain_ref, w_hbm, out_ref,
    src, recv, local_in, vt, scores, ostage, local_out, orecv, wall, gate, mixed, sig, gated, acc,
    load_sem, gate_sem, wload_sem, kv_send, kv_recv, q_send, q_recv, o_send, o_recv, l_send, l_recv, lo_send,
    wz_send, wz_recv, wy_send, wy_recv, wx_send, wx_recv, wp_send, wp_recv,
):
    me = lax.axis_index("sp")
    dp = lax.axis_index("dp")
    z, y = me // NY, lax.rem(me, NY)
    x, core = dp // 2, lax.rem(dp, 2)
    first_slab = z == 0
    later_slab = z > 0

    def plane_peer(dz, dy):
        return lax.rem(z + dz, NZ) * NY + lax.rem(y + dy, NY)

    def x_peer(dx):
        return lax.rem(x + dx, NX) * 2 + core

    partner = x * 2 + 1 - core
    barrier = pltpu.get_barrier_semaphore()

    @pl.loop(1, NSP)
    def _(d):
        pl.semaphore_signal(
            barrier, inc=1, device_id=(lax.rem(me + d, NSP), dp), device_id_type=MESH
        )

    @pl.loop(1, NX)
    def _(d):
        pl.semaphore_signal(barrier, inc=1, device_id=(me, x_peer(d)), device_id_type=MESH)

    pl.semaphore_signal(barrier, inc=1, device_id=(me, partner), device_id_type=MESH)

    def local(a, b, sem):
        copy = pltpu.make_async_copy(a, b, sem)
        copy.start()
        return copy

    def remote(a, b, send, rcv, sp, d):
        copy = pltpu.make_async_remote_copy(
            src_ref=a, dst_ref=b, send_sem=send, recv_sem=rcv, device_id=(sp, d), device_id_type=MESH
        )
        copy.start()

    def drain(ref, sem):
        pltpu.make_async_copy(ref, ref, sem).wait()

    tensors = (k_hbm, v_hbm, q_hbm)
    w_load = local(w_hbm, wall.at[dp, z, y], wload_sem)
    loads = []
    for i in range(2):
        loads.append(
            [local(t.at[i], src.at[i, :, :, n], load_sem.at[i, n]) for n, t in enumerate(tensors)]
        )
        for n, t in enumerate(tensors):
            local(
                t.at[i, z, y],
                recv.at[i, me, n],
                kv_recv.at[i] if n < 2 else q_recv.at[i, z],
            )
    @pl.when(first_slab)
    def _():
        for i in range(LOCAL):
            for n, t in enumerate(tensors):
                local(t.at[i, pl.ds(1, NZ - 1), y], local_in.at[i, :, y, n], l_recv.at[i])

    gate_load = local(gate_hbm, gate, gate_sem)

    w_load.wait()
    for i in range(2):
        for copy in loads[i]:
            copy.wait()
    pl.semaphore_wait(barrier, NSP - 1 + NX - 1 + 1)

    def send_weights_z(row, dz, rcv):
        block = wall.at[dp, row, y]
        remote(block, block, wz_send, rcv, plane_peer(dz, 0), dp)

    def send_weights_x(col):
        rows = wall.at[dp, :, col]

        @pl.loop(1, NX)
        def _(d):
            remote(rows, rows, wx_send, wx_recv, me, x_peer(d))

    def send_kv(i, start, stop):
        @pl.loop(start, stop)
        def _(n):
            spot = lax.rem(5 * n, NSP)
            to = plane_peer(spot // NY, lax.rem(spot, NY))
            remote(
                src.at[i, to // NY, lax.rem(to, NY), pl.ds(0, 2)],
                recv.at[i, me, pl.ds(0, 2)],
                kv_send,
                kv_recv.at[i],
                to,
                dp,
            )

    def send_q(i):
        @pl.loop(1, jnp.where(first_slab, NY, NSP) if i < LOCAL else NSP)
        def _(n):
            to = plane_peer(slab_offset(n // NY), lax.rem(n, NY))
            remote(
                src.at[i, to // NY, lax.rem(to, NY), 2],
                recv.at[i, me, 2],
                q_send,
                q_recv.at[i, z],
                to,
                dp,
            )

    def send_local(i):
        @pl.when(first_slab)
        def _():
            @pl.loop(1, NY)
            def _(d):
                to = lax.rem(y + d, NY)
                remote(
                    src.at[i, pl.ds(1, NZ - 1), to],
                    local_in.at[i, :, y],
                    l_send,
                    l_recv.at[i],
                    to,
                    dp,
                )

    for dz in (1, NZ - 1, 2, NZ - 2):
        send_weights_z(z, dz, wz_recv.at[0])
    send_kv(0, 1, AHEAD_1)
    drain(wall.at[dp, pl.ds(0, 4), y], wz_recv.at[0])
    before, after = lax.rem(z + NZ - 2, NZ), lax.rem(z + 2, NZ)
    send_weights_z(before, 1, wz_recv.at[1])
    send_weights_z(before, 2, wz_recv.at[1])
    send_weights_z(after, NZ - 1, wz_recv.at[1])
    send_kv(0, AHEAD_1, AHEAD_2)
    drain(wall.at[dp, pl.ds(0, 3), y], wz_recv.at[1])

    @pl.loop(1, NY)
    def _(d):
        mine = wall.at[dp, :, y]
        remote(mine, mine, wy_send, wy_recv, plane_peer(0, d), dp)

    send_weights_x(y)
    send_kv(0, AHEAD_2, NSP)
    send_q(0)
    send_local(0)

    gate_load.wait()

    @pl.loop(0, 16)
    def _(n):
        rows = pl.ds(pl.multiple_of(4 * n, 4), 4)
        mixed[rows] = jax.nn.sigmoid(gate[rows].astype(F32))

    for b in range(4):
        sig[b] = mixed[:, b]

    drain(wall.at[dp, :, pl.ds(0, NY - 1)], wy_recv)

    @pl.loop(1, NY)
    def _(d):
        send_weights_x(lax.rem(y + d, NY))

    remote(wall.at[dp], wall.at[dp], wp_send, wp_recv, me, partner)
    send_kv(1, 1, NSP)
    send_q(1)

    gain = gain_ref[...]
    lam = lam_ref[lax.rem(me, 16)]

    @pl.loop(0, 2)
    def _(item):
        drain(recv.at[0, :, pl.ds(0, 2)], kv_recv.at[item])
        kvq = recv.at[item]

        @pl.loop(0, NZ)
        def _(b):
            transpose_values(kvq, vt, b)

        @pl.loop(0, NZ)
        def _(step):
            slab = lax.rem(z + NZ - slab_offset(step), NZ)
            here = jnp.logical_or(first_slab, slab > 0)

            @pl.when(jnp.logical_or(here, item >= LOCAL))
            def _():
                drain(recv.at[0, pl.ds(0, NY), 2], q_recv.at[item, slab])
                for s in range(NZ):

                    @pl.when(slab == s)
                    def _():
                        slab_attention(s, kvq, vt, scores, ostage.at[item], lam, gain)

                @pl.loop(0, NY)
                def _(n):
                    to = slab * NY + n

                    @pl.when(to == me)
                    def _():
                        orecv[item, z, y] = ostage[item, me]

                    @pl.when(to != me)
                    def _():
                        remote(
                            ostage.at[item, to],
                            orecv.at[item, z, y],
                            o_send,
                            o_recv.at[item, z],
                            to,
                            dp,
                        )

            @pl.when(jnp.logical_and(item == 1, step == 2))
            def _():
                drain(wall.at[pl.ds(0, NX - 1)], wx_recv)

                @pl.loop(1, NX)
                def _(d):
                    rows = wall.at[x_peer(d)]
                    remote(rows, rows, wp_send, wp_recv, me, partner)

        @pl.when(jnp.logical_and(first_slab, item == 0))
        def _():
            @pl.loop(0, LOCAL)
            def _(i):
                drain(local_in.at[0], l_recv.at[i])

                @pl.loop(0, NZ - 1)
                def _(j):
                    block = local_in.at[i, j]
                    transpose_values(block, vt, 0)
                    lam_j = lam_ref[lax.rem(NY * (j + 1) + y, 16)]
                    slab_attention(0, block, vt, scores, local_out.at[i, j], lam_j, gain)
                    orecv[i, j + 1, y] = local_out[i, j, y]

                @pl.loop(1, NY)
                def _(d):
                    to = lax.rem(y + d, NY)
                    remote(
                        local_out.at[i, :, to],
                        orecv.at[i, pl.ds(1, NZ - 1), y],
                        lo_send,
                        o_recv.at[i, z],
                        to,
                        dp,
                    )

    drain(wall.at[pl.ds(0, NX)], wp_recv)
    acc[...] = jnp.zeros_like(acc)

    @pl.loop(0, NZ)
    def _(step):
        i = step // 4
        j = lax.rem(z + step, 4)
        near = jnp.logical_and(first_slab, i < LOCAL)
        far = jnp.logical_or(later_slab, i >= LOCAL)
        for b in range(2):
            rank = j + 4 * b

            @pl.when(jnp.logical_and(near, rank == 0))
            def _():
                drain(orecv.at[0, :, pl.ds(0, NY - 1)], o_recv.at[i, rank])

            @pl.when(jnp.logical_and(far, rank == z))
            def _():
                drain(orecv.at[0, 0, pl.ds(0, NY - 1)], o_recv.at[i, rank])

            @pl.when(jnp.logical_and(far, rank != z))
            def _():
                drain(orecv.at[0, 0], o_recv.at[i, rank])

            for h in range(4):
                cols = pl.ds(pl.multiple_of(512 * j + 128 * h, 128), 128)
                gated[pl.ds(64 * b, 64), pl.ds(128 * h, 128)] = (
                    sig[2 * i + b, :, cols] * orecv[i, rank, h].astype(F32)
                ).astype(BF16)
        for c in range(NDP):
            acc[i, :, pl.ds(256 * c, 256)] += jnp.dot(
                gated[...], wall[c, pl.ds(2 * j, 2)].reshape(512, 256), preferred_element_type=F32
            )

    out_ref[...] = acc[...].astype(BF16)

    drain(recv.at[:, pl.ds(0, NSP - 1), pl.ds(0, 2)], kv_send)
    for i in range(2):

        @pl.when(first_slab)
        def _():
            drain(recv.at[0, pl.ds(0, NY - 1 if i < LOCAL else NSP - 1), 2], q_send)
            drain(ostage.at[0, pl.ds(0, NSP - 1)], o_send)
            if i < LOCAL:
                drain(local_in.at[0, :, pl.ds(0, NY - 1)], l_send)
                drain(local_out.at[0, :, pl.ds(0, NY - 1)], lo_send)

        @pl.when(later_slab)
        def _():
            drain(recv.at[0, pl.ds(0, NSP - 1), 2], q_send)
            drain(ostage.at[0, pl.ds(0, NSP - 1 - (NY if i < LOCAL else 0))], o_send)

    drain(wall.at[dp, pl.ds(0, NZ - 1), y], wz_send)
    drain(wall.at[dp, :, pl.ds(0, NY - 1)], wy_send)
    drain(wall.at[pl.ds(0, NX - 1)], wx_send)
    drain(wall.at[pl.ds(0, NX)], wp_send)


def on_device(queries, key_maps, value_rows, gate_logits, mix_lambda, head_gain, out_weight):
    any_spec = pl.BlockSpec(memory_space=pl.ANY)
    dma = pltpu.SemaphoreType.DMA
    out = pl.pallas_call(
        kernel,
        out_shape=jax.ShapeDtypeStruct((2, 128, 2048), BF16),
        in_specs=[any_spec, any_spec, any_spec, any_spec, pl.BlockSpec(memory_space=pltpu.SMEM),
                  pl.BlockSpec(memory_space=pltpu.VMEM), any_spec],
        out_specs=pl.BlockSpec(memory_space=pltpu.VMEM),
        scratch_shapes=[
            pltpu.VMEM((2, NZ, NY, 3, 64, 128), BF16),
            pltpu.VMEM((2, NSP, 3, 64, 128), BF16),
            pltpu.VMEM((LOCAL, NZ - 1, NY, 3, 64, 128), BF16),
            pltpu.VMEM((128, 2048), BF16),
            pltpu.VMEM((2, 2048, 256), F32),
            pltpu.VMEM((2, NSP, 64, 128), BF16),
            pltpu.VMEM((LOCAL, NZ - 1, NY, 64, 128), BF16),
            pltpu.VMEM((2, NZ, NY, 64, 128), BF16),
            pltpu.VMEM((NDP, NZ, NY, 64, 256), BF16),
            pltpu.VMEM((64, 4, 2048), BF16),
            pltpu.VMEM((64, 4, 2048), F32),
            pltpu.VMEM((4, 64, 2048), F32),
            pltpu.VMEM((128, 512), BF16),
            pltpu.VMEM((2, 128, 2048), F32),
            dma((2, 3)), dma, dma, dma, dma((2,)), dma, dma((2, NZ)), dma, dma((2, NZ)), dma, dma((LOCAL,)), dma,
            dma, dma((2,)), dma, dma, dma, dma, dma, dma,
        ],
        compiler_params=pltpu.CompilerParams(
            collective_id=0, has_side_effects=True, vmem_limit_bytes=60 << 20
        ),
        name="fused_layer",
    )(
        queries.reshape(2, NZ, NY, 64, 128),
        key_maps.reshape(2, NZ, NY, 64, 128),
        value_rows.reshape(2, NZ, NY, 64, 128),
        gate_logits,
        mix_lambda,
        head_gain.reshape(1, 128),
        out_weight,
    )
    return jnp.transpose(out.reshape(4, 64, 2048), (1, 0, 2))


def solution(mesh):
    return jax.shard_map(
        on_device,
        mesh=mesh,
        in_specs=(
            P("dp", None, "sp", None),
            P("dp", None, "sp", None),
            P("dp", None, "sp", None),
            P("sp", "dp", None),
            P(),
            P(),
            P("sp", "dp"),
        ),
        out_specs=P("sp", "dp", None),
        check_vma=False,
    )
```

```python
import math

import jax
import jax.numpy as jnp
from jax import lax
from jax.experimental import pallas as pl
from jax.experimental.pallas import tpu as pltpu
from jax.sharding import PartitionSpec as P

MESH = pl.DeviceIdType.MESH
HEAD_DIM = 64
NZ, NY, NX = 8, 4, 4
NSP, NDP = NZ * NY, 2 * NX
AHEAD_1, AHEAD_2 = 8, 14
LOCAL = 1
EXP_SCALE = HEAD_DIM ** (-0.5) * math.log2(math.e)
F32, BF16 = jnp.float32, jnp.bfloat16


def slab_offset(step):
    return step // 2 + 4 * (step % 2)


def transpose_values(kvq, vt, block):
    cols = pl.ds(pl.multiple_of(256 * block, 256), 256)
    vt[:, cols] = kvq[pl.ds(NY * block, NY), 1].reshape(256, 128).T


def slab_attention(s, kvq, vt, scores, out, lam, gain):
    lane = lax.broadcasted_iota(jnp.int32, (128, 128), 1)
    half_lane = lax.rem(lax.broadcasted_iota(jnp.int32, (64, 256), 1), 128)
    for h in range(2):
        first = NY * s + 2 * h
        q = kvq[pl.ds(first, 2), 2].reshape(128, 128)
        zero = jnp.zeros_like(q)
        qm = jnp.concatenate(
            [jnp.where(lane < HEAD_DIM, q, zero), jnp.where(lane >= HEAD_DIM, q, zero)], axis=0
        )
        chunks = first + 2
        blocks = []
        at = 0
        while at < chunks:
            size = min(4, chunks - at)
            blocks.append((at, size))
            at += size
        highest = jnp.full((8, 256), -1e30, F32)
        for at, size in blocks:
            rows = 64 * size
            keys = kvq[pl.ds(at, size), 0].reshape(rows, 128)
            st = lax.dot_general(
                keys, qm, (((1,), (1,)), ((), ())), preferred_element_type=F32
            )
            if at + size == chunks:
                tail = jnp.where(half_lane < 64, -1e30, st[rows - 64 :])
                st = jnp.concatenate([st[: rows - 64], tail], axis=0)
            scores[h, pl.ds(64 * at, rows)] = st
            highest = jnp.maximum(highest, jnp.max(st.reshape(rows // 8, 8, 256), axis=0))
        highest = jnp.max(highest, axis=0, keepdims=True)
        summed = jnp.zeros((8, 256), F32)
        mapped = jnp.zeros((128, 256), F32)
        for at, size in blocks:
            rows = 64 * size
            weights = jnp.exp2((scores[h, pl.ds(64 * at, rows)] - highest) * EXP_SCALE)
            summed = summed + jnp.sum(weights.reshape(rows // 8, 8, 256), axis=0)
            mapped = mapped + jnp.dot(
                vt[:, pl.ds(64 * at, rows)], weights.astype(BF16), preferred_element_type=F32
            )
        mapped = mapped * (1.0 / jnp.sum(summed, axis=0, keepdims=True))
        combined = mapped[:, :128] - lam * mapped[:, 128:]
        mean_sq = jnp.sum(combined * combined, axis=0, keepdims=True) * (1.0 / 128)
        normed = (combined * lax.rsqrt(mean_sq + 1e-5)).T * gain
        out[pl.ds(first, 2)] = normed.astype(BF16).reshape(2, 64, 128)


def kernel(
    q_hbm, k_hbm, v_hbm, gate_hbm, lam_ref, gain_ref, w_hbm, out_ref,
    src, recv, local_in, vt, scores, ostage, local_out, orecv, wall, gate, mixed, sig, gated, acc,
    load_sem, gate_sem, wload_sem, kv_send, kv_recv, q_send, q_recv, o_send, o_recv, l_send, l_recv, lo_send,
    wz_send, wz_recv, wy_send, wy_recv, wx_send, wx_recv, wp_send, wp_recv,
):
    me = lax.axis_index("sp")
    dp = lax.axis_index("dp")
    z, y = me // NY, lax.rem(me, NY)
    x, core = dp // 2, lax.rem(dp, 2)
    first_slab = z == 0
    later_slab = z > 0

    def plane_peer(dz, dy):
        return lax.rem(z + dz, NZ) * NY + lax.rem(y + dy, NY)

    def x_peer(dx):
        return lax.rem(x + dx, NX) * 2 + core

    partner = x * 2 + 1 - core
    barrier = pltpu.get_barrier_semaphore()

    @pl.loop(1, NSP)
    def _(d):
        pl.semaphore_signal(
            barrier, inc=1, device_id=(lax.rem(me + d, NSP), dp), device_id_type=MESH
        )

    @pl.loop(1, NX)
    def _(d):
        pl.semaphore_signal(barrier, inc=1, device_id=(me, x_peer(d)), device_id_type=MESH)

    pl.semaphore_signal(barrier, inc=1, device_id=(me, partner), device_id_type=MESH)

    def local(a, b, sem):
        copy = pltpu.make_async_copy(a, b, sem)
        copy.start()
        return copy

    def remote(a, b, send, rcv, sp, d):
        copy = pltpu.make_async_remote_copy(
            src_ref=a, dst_ref=b, send_sem=send, recv_sem=rcv, device_id=(sp, d), device_id_type=MESH
        )
        copy.start()

    def drain(ref, sem):
        pltpu.make_async_copy(ref, ref, sem).wait()

    tensors = (k_hbm, v_hbm, q_hbm)
    w_load = local(w_hbm, wall.at[dp, z, y], wload_sem)
    loads = []
    for i in range(2):
        loads.append(
            [local(t.at[i], src.at[i, :, :, n], load_sem.at[i, n]) for n, t in enumerate(tensors)]
        )
        for n, t in enumerate(tensors):
            local(
                t.at[i, z, y],
                recv.at[i, me, n],
                kv_recv.at[i] if n < 2 else q_recv.at[i, z],
            )
    @pl.when(first_slab)
    def _():
        for i in range(LOCAL):
            for n, t in enumerate(tensors):
                local(t.at[i, pl.ds(1, NZ - 1), y], local_in.at[i, :, y, n], l_recv.at[i])

    gate_load = local(gate_hbm, gate, gate_sem)

    w_load.wait()
    for i in range(2):
        for copy in loads[i]:
            copy.wait()
    pl.semaphore_wait(barrier, NSP - 1 + NX - 1 + 1)

    def send_weights_z(row, dz, rcv):
        block = wall.at[dp, row, y]
        remote(block, block, wz_send, rcv, plane_peer(dz, 0), dp)

    def send_weights_x(col):
        rows = wall.at[dp, :, col]

        @pl.loop(1, NX)
        def _(d):
            remote(rows, rows, wx_send, wx_recv, me, x_peer(d))

    def send_kv(i, start, stop):
        @pl.loop(start, stop)
        def _(n):
            spot = lax.rem(5 * n, NSP)
            to = plane_peer(spot // NY, lax.rem(spot, NY))
            remote(
                src.at[i, to // NY, lax.rem(to, NY), pl.ds(0, 2)],
                recv.at[i, me, pl.ds(0, 2)],
                kv_send,
                kv_recv.at[i],
                to,
                dp,
            )

    def send_q(i):
        @pl.loop(1, jnp.where(first_slab, NY, NSP) if i < LOCAL else NSP)
        def _(n):
            to = plane_peer(slab_offset(n // NY), lax.rem(n, NY))
            remote(
                src.at[i, to // NY, lax.rem(to, NY), 2],
                recv.at[i, me, 2],
                q_send,
                q_recv.at[i, z],
                to,
                dp,
            )

    def send_local(i):
        @pl.when(first_slab)
        def _():
            @pl.loop(1, NY)
            def _(d):
                to = lax.rem(y + d, NY)
                remote(
                    src.at[i, pl.ds(1, NZ - 1), to],
                    local_in.at[i, :, y],
                    l_send,
                    l_recv.at[i],
                    to,
                    dp,
                )

    for dz in (1, NZ - 1, 2, NZ - 2):
        send_weights_z(z, dz, wz_recv.at[0])
    send_kv(0, 1, AHEAD_1)
    drain(wall.at[dp, pl.ds(0, 4), y], wz_recv.at[0])
    before, after = lax.rem(z + NZ - 2, NZ), lax.rem(z + 2, NZ)
    send_weights_z(before, 1, wz_recv.at[1])
    send_weights_z(before, 2, wz_recv.at[1])
    send_weights_z(after, NZ - 1, wz_recv.at[1])
    send_kv(0, AHEAD_1, AHEAD_2)
    drain(wall.at[dp, pl.ds(0, 3), y], wz_recv.at[1])

    @pl.loop(1, NY)
    def _(d):
        mine = wall.at[dp, :, y]
        remote(mine, mine, wy_send, wy_recv, plane_peer(0, d), dp)

    send_weights_x(y)
    send_kv(0, AHEAD_2, NSP)
    send_q(0)
    send_local(0)

    gate_load.wait()

    @pl.loop(0, 16)
    def _(n):
        rows = pl.ds(pl.multiple_of(4 * n, 4), 4)
        mixed[rows] = jax.nn.sigmoid(gate[rows].astype(F32))

    for b in range(4):
        sig[b] = mixed[:, b]

    drain(wall.at[dp, :, pl.ds(0, NY - 1)], wy_recv)

    @pl.loop(1, NY)
    def _(d):
        send_weights_x(lax.rem(y + d, NY))

    remote(wall.at[dp], wall.at[dp], wp_send, wp_recv, me, partner)
    send_kv(1, 1, NSP)
    send_q(1)

    gain = gain_ref[...]
    lam = lam_ref[lax.rem(me, 16)]

    @pl.loop(0, 2)
    def _(item):
        drain(recv.at[0, :, pl.ds(0, 2)], kv_recv.at[item])
        kvq = recv.at[item]

        @pl.loop(0, NZ)
        def _(b):
            transpose_values(kvq, vt, b)

        @pl.loop(0, NZ)
        def _(step):
            slab = lax.rem(z + NZ - slab_offset(step), NZ)
            here = jnp.logical_or(first_slab, slab > 0)

            @pl.when(jnp.logical_or(here, item >= LOCAL))
            def _():
                drain(recv.at[0, pl.ds(0, NY), 2], q_recv.at[item, slab])
                for s in range(NZ):

                    @pl.when(slab == s)
                    def _():
                        slab_attention(s, kvq, vt, scores, ostage.at[item], lam, gain)

                @pl.loop(0, NY)
                def _(n):
                    to = slab * NY + n

                    @pl.when(to == me)
                    def _():
                        orecv[item, z, y] = ostage[item, me]

                    @pl.when(to != me)
                    def _():
                        remote(
                            ostage.at[item, to],
                            orecv.at[item, z, y],
                            o_send,
                            o_recv.at[item, z],
                            to,
                            dp,
                        )

            @pl.when(jnp.logical_and(item == 1, step == 4))
            def _():
                drain(wall.at[pl.ds(0, NX - 1)], wx_recv)

                @pl.loop(1, NX)
                def _(d):
                    rows = wall.at[x_peer(d)]
                    remote(rows, rows, wp_send, wp_recv, me, partner)

        @pl.when(jnp.logical_and(first_slab, item == 0))
        def _():
            @pl.loop(0, LOCAL)
            def _(i):
                drain(local_in.at[0], l_recv.at[i])

                @pl.loop(0, NZ - 1)
                def _(j):
                    block = local_in.at[i, j]
                    transpose_values(block, vt, 0)
                    lam_j = lam_ref[lax.rem(NY * (j + 1) + y, 16)]
                    slab_attention(0, block, vt, scores, local_out.at[i, j], lam_j, gain)
                    orecv[i, j + 1, y] = local_out[i, j, y]

                @pl.loop(1, NY)
                def _(d):
                    to = lax.rem(y + d, NY)
                    remote(
                        local_out.at[i, :, to],
                        orecv.at[i, pl.ds(1, NZ - 1), y],
                        lo_send,
                        o_recv.at[i, z],
                        to,
                        dp,
                    )

    drain(wall.at[pl.ds(0, NX)], wp_recv)
    acc[...] = jnp.zeros_like(acc)

    @pl.loop(0, NZ)
    def _(step):
        i = step // 4
        j = lax.rem(z + step, 4)
        near = jnp.logical_and(first_slab, i < LOCAL)
        far = jnp.logical_or(later_slab, i >= LOCAL)
        for b in range(2):
            rank = j + 4 * b

            @pl.when(jnp.logical_and(near, rank == 0))
            def _():
                drain(orecv.at[0, :, pl.ds(0, NY - 1)], o_recv.at[i, rank])

            @pl.when(jnp.logical_and(far, rank == z))
            def _():
                drain(orecv.at[0, 0, pl.ds(0, NY - 1)], o_recv.at[i, rank])

            @pl.when(jnp.logical_and(far, rank != z))
            def _():
                drain(orecv.at[0, 0], o_recv.at[i, rank])

            for h in range(4):
                cols = pl.ds(pl.multiple_of(512 * j + 128 * h, 128), 128)
                gated[pl.ds(64 * b, 64), pl.ds(128 * h, 128)] = (
                    sig[2 * i + b, :, cols] * orecv[i, rank, h].astype(F32)
                ).astype(BF16)
        for c in range(NDP):
            acc[i, :, pl.ds(256 * c, 256)] += jnp.dot(
                gated[...], wall[c, pl.ds(2 * j, 2)].reshape(512, 256), preferred_element_type=F32
            )

    out_ref[...] = acc[...].astype(BF16)

    drain(recv.at[:, pl.ds(0, NSP - 1), pl.ds(0, 2)], kv_send)
    for i in range(2):

        @pl.when(first_slab)
        def _():
            drain(recv.at[0, pl.ds(0, NY - 1 if i < LOCAL else NSP - 1), 2], q_send)
            drain(ostage.at[0, pl.ds(0, NSP - 1)], o_send)
            if i < LOCAL:
                drain(local_in.at[0, :, pl.ds(0, NY - 1)], l_send)
                drain(local_out.at[0, :, pl.ds(0, NY - 1)], lo_send)

        @pl.when(later_slab)
        def _():
            drain(recv.at[0, pl.ds(0, NSP - 1), 2], q_send)
            drain(ostage.at[0, pl.ds(0, NSP - 1 - (NY if i < LOCAL else 0))], o_send)

    drain(wall.at[dp, pl.ds(0, NZ - 1), y], wz_send)
    drain(wall.at[dp, :, pl.ds(0, NY - 1)], wy_send)
    drain(wall.at[pl.ds(0, NX - 1)], wx_send)
    drain(wall.at[pl.ds(0, NX)], wp_send)


def on_device(queries, key_maps, value_rows, gate_logits, mix_lambda, head_gain, out_weight):
    any_spec = pl.BlockSpec(memory_space=pl.ANY)
    dma = pltpu.SemaphoreType.DMA
    out = pl.pallas_call(
        kernel,
        out_shape=jax.ShapeDtypeStruct((2, 128, 2048), BF16),
        in_specs=[any_spec, any_spec, any_spec, any_spec, pl.BlockSpec(memory_space=pltpu.SMEM),
                  pl.BlockSpec(memory_space=pltpu.VMEM), any_spec],
        out_specs=pl.BlockSpec(memory_space=pltpu.VMEM),
        scratch_shapes=[
            pltpu.VMEM((2, NZ, NY, 3, 64, 128), BF16),
            pltpu.VMEM((2, NSP, 3, 64, 128), BF16),
            pltpu.VMEM((LOCAL, NZ - 1, NY, 3, 64, 128), BF16),
            pltpu.VMEM((128, 2048), BF16),
            pltpu.VMEM((2, 2048, 256), F32),
            pltpu.VMEM((2, NSP, 64, 128), BF16),
            pltpu.VMEM((LOCAL, NZ - 1, NY, 64, 128), BF16),
            pltpu.VMEM((2, NZ, NY, 64, 128), BF16),
            pltpu.VMEM((NDP, NZ, NY, 64, 256), BF16),
            pltpu.VMEM((64, 4, 2048), BF16),
            pltpu.VMEM((64, 4, 2048), F32),
            pltpu.VMEM((4, 64, 2048), F32),
            pltpu.VMEM((128, 512), BF16),
            pltpu.VMEM((2, 128, 2048), F32),
            dma((2, 3)), dma, dma, dma, dma((2,)), dma, dma((2, NZ)), dma, dma((2, NZ)), dma, dma((LOCAL,)), dma,
            dma, dma((2,)), dma, dma, dma, dma, dma, dma,
        ],
        compiler_params=pltpu.CompilerParams(
            collective_id=0, has_side_effects=True, vmem_limit_bytes=60 << 20
        ),
        name="fused_layer",
    )(
        queries.reshape(2, NZ, NY, 64, 128),
        key_maps.reshape(2, NZ, NY, 64, 128),
        value_rows.reshape(2, NZ, NY, 64, 128),
        gate_logits,
        mix_lambda,
        head_gain.reshape(1, 128),
        out_weight,
    )
    return jnp.transpose(out.reshape(4, 64, 2048), (1, 0, 2))


def solution(mesh):
    return jax.shard_map(
        on_device,
        mesh=mesh,
        in_specs=(
            P("dp", None, "sp", None),
            P("dp", None, "sp", None),
            P("dp", None, "sp", None),
            P("sp", "dp", None),
            P(),
            P(),
            P("sp", "dp"),
        ),
        out_specs=P("sp", "dp", None),
        check_vma=False,
    )
```
